32 devices in a mesh: sp: 4 (over y, x), tp: 8 (over z, core).
Axes of the slice: x: 2, y: 2, z: 4, core: 2. Of those that a mesh axis runs over, the one named last changes fastest.
Arguments:
- query_rows: bfloat16 [8192, 1024], P('sp', 'tp'), may hold values from -6 to 6
- key_rows: bfloat16 [8192, 1024], P('sp', 'tp'), may hold values from -6 to 6
- value_rows: bfloat16 [8192, 1024], P('sp', 'tp'), may hold values from -6 to 6
- gate_rows: bfloat16 [8192, 1024], P('sp', 'tp'), may hold values from -6 to 6
- log_decay: float32 [16, 8192], P('tp', 'sp'), may hold values from -1 to 0
- residual: bfloat16 [8192, 2048], P(('sp', 'tp')), may hold values from -6 to 6
- head_gain: float32 [1024], P('tp'), may hold values from 0.1 to 1.9
- out_weight: bfloat16 [1024, 2048], P(None, 'tp'), may hold values from -0.1875 to 0.1875
- norm_gain: float32 [2048], replicated, may hold values from 0.1 to 1.9
- expert_ids: int32 [8192, 2], P(('sp', 'tp')), may hold values from 0 to 3, all different within a row; in each aligned block of 256 rows (0 to 255, 256 to 511, ...) at most 192 rows name the same one
- route_weights: float32 [8192, 2], P(('sp', 'tp')), may hold values from 0.2 to 1
- expert_gate: bfloat16 [2048, 4096], P(None, ('sp', 'tp')), may hold values from -0.125 to 0.125
- expert_up: bfloat16 [2048, 4096], P(None, ('sp', 'tp')), may hold values from -0.125 to 0.125
- expert_down: bfloat16 [2048, 4096], P(None, ('sp', 'tp')), may hold values from -0.1875 to 0.1875
- shared_gate: bfloat16 [2048, 512], replicated, may hold values from -0.125 to 0.125
- shared_up: bfloat16 [2048, 512], replicated, may hold values from -0.125 to 0.125
- shared_down: bfloat16 [2048, 512], replicated, may hold values from -0.25 to 0.25
Outputs:
- result: bfloat16 [8192, 2048], P(('sp', 'tp'))
The draws below stay inside these ranges and needn't reach their ends.
Inputs may be any that keep to these rules, and one draw needn't show every extreme that they name: `expert_ids`: each row names 2 different experts. Within the rows of one device (aligned blocks of 256 rows) no expert is named by more than 192 rows, and in some block an expert is named by exactly 192 rows.
All inputs are finite; a program needn't handle non-finite values.
Results may differ from the reference program's by a relative error of at most 0.0075.
Values may be sent and summed in bfloat16 or wider, within the bound.
A program may use at most 128 MiB of HBM per device.

```python
import math
import jax
import jax.numpy as jnp
import numpy as np
from jax import lax

D = 2048
HEADS = 16
HEAD = 64
HW = 1024
FF = 1024
SH = 512
TOPK = 2
SPAN = 512
TOK_DEV = 256
TOKENS = 8192
SPECIALISTS = 4
CAP = 192


def draw_log_decay(key, part):
    streams = jax.random.split(key, 6)
    slow_share = 0.5
    sequence_ordinals = jnp.arange(TOKENS, dtype=jnp.int32)
    chance = jax.random.uniform(streams[0], (HEADS,))
    slow = chance < slow_share
    fast_rate = jnp.exp(jax.random.uniform(streams[1], (HEADS,), minval=jnp.log(1.0 / 100.0), maxval=jnp.log(1.0 / 30.0)))
    slow_rate = jnp.exp(jax.random.uniform(streams[2], (HEADS,), minval=jnp.log(0.1), maxval=jnp.log(0.8))) / TOKENS
    rate = jnp.where(slow, slow_rate, fast_rate)
    factor = jnp.exp(jax.random.uniform(streams[3], (16,), minval=jnp.log(0.25), maxval=0.0))
    individual_slot_factor = factor[sequence_ordinals * 16 // TOKENS]
    constant_shrinkage = -rate[:, None] * individual_slot_factor[None, :]
    shifted_locations = jax.random.randint(streams[4], (HEADS, 2), 0, TOKENS)
    stack_level = jax.random.uniform(streams[5], (HEADS, 2), minval=jnp.log(0.5), maxval=jnp.log(0.8))
    segment_bundles = jnp.sum(jnp.where(sequence_ordinals[None, None, :] == shifted_locations[:, :, None], stack_level[:, :, None], 0.0), axis=1)
    return (constant_shrinkage + segment_bundles).astype(jnp.float32)


def block_levels(stream_key, dims, cuts, low, largest):
    gain = 1.0
    for dim, parts in cuts:
        heights = jax.random.uniform(jax.random.fold_in(jax.random.fold_in(stream_key, 6), dim), (parts,), jnp.float32, low / len(cuts), largest / len(cuts))
        gain = gain * jnp.repeat(jnp.exp(heights), dims[dim] // parts).reshape((-1,) + (1,) * (len(dims) - 1 - dim))
    return gain


def deal_out(rng, own, number, rows, count, top, reach, lean):
    sequence = jax.random.permutation(rng, count)
    crowded, common = load_shares(count, rows * top, reach, lean, True), load_shares(count, rows * top, reach, lean, False)
    places = jnp.arange(count)

    def named(lengths, offset_by):
        used = int((lengths > 0).sum())
        fixed = max(1, used // 4)
        moved = fixed + (places - fixed + offset_by * (used - fixed)) % max(1, count - fixed)
        return jnp.zeros((count,), jnp.int32).at[sequence[jnp.where(places < fixed, places, moved)]].set(jnp.asarray(lengths, jnp.int32))

    lengths = jnp.where(number % 4 == 0, named(crowded, number // 4), named(common, number - number // 4 - 1))
    mixed = jax.random.permutation(jax.random.fold_in(own, 3), count)
    giver, sink = mixed[0:count // 2 * 2:2], mixed[1:count // 2 * 2:2]
    slack = jnp.minimum(lengths[giver] - 1, reach - lengths[sink]) // 2
    slack = jnp.where((giver == sequence[0]) | (sink == sequence[0]) | (lengths[sink] == 0), 0, jnp.maximum(slack, 0))
    moved = jax.random.randint(jax.random.fold_in(own, 4), (count // 2,), 0, 1 << 20) % (slack + 1)
    lengths = lengths.at[giver].add(-moved).at[sink].add(moved)
    labels = jnp.searchsorted(jnp.cumsum(lengths), jnp.arange(rows * top), side="right").astype(jnp.int32)
    table = labels.reshape(top, rows).T
    table = table[jax.random.permutation(jax.random.fold_in(own, 1), rows)]
    offset_by = jax.random.randint(jax.random.fold_in(own, 2), (rows, 1), 0, top)
    return jnp.take_along_axis(table, (jnp.arange(top)[None, :] + offset_by) % top, axis=1)


def load_shares(number_of, total, reach, slope, full):
    portions = [(1 << 20) // math.isqrt(standing ** slope) + 1 for standing in range(1, number_of + 1)]
    largest = reach if full else min(reach, max(-(-total // number_of), total * portions[0] // sum(portions)))
    least = 1 if total - largest >= number_of - 1 else 0
    counts, rest = [largest] + [least] * (number_of - 1), total - largest - least * (number_of - 1)
    while rest > 0:
        candidates = [i for i in range(1, number_of) if counts[i] < largest] or [i for i in range(1, number_of) if counts[i] < reach]
        whole, budget = sum([portions[i] for i in candidates]), rest
        for i in candidates:
            addition = min(reach - counts[i], max(1, budget * portions[i] // whole), rest)
            counts[i] = counts[i] + addition
            rest = rest - addition
    return np.array(counts)


def centred(key, dims, scale, limit, pieces=(), kind=jnp.bfloat16):
    loudness = block_levels(key, dims, pieces, -0.22, 0.18) if pieces else 1.0
    array = jax.random.normal(key, dims, jnp.float32) * scale * loudness
    return jnp.minimum(jnp.maximum(array, -limit), limit).astype(kind)


def setup_inputs(seed: int = 0) -> dict:
    streams_of = jax.random.split(jax.random.key(seed), 18)
    query_rows = centred(streams_of[0], (TOKENS, HW), 1.0, 6.0, ((0, 4), (1, 8)))
    key_rows = centred(streams_of[1], (TOKENS, HW), 1.0, 6.0, ((0, 4), (1, 8)))
    value_rows = centred(streams_of[2], (TOKENS, HW), 1.0, 6.0, ((0, 4), (1, 8)))
    gate_rows = centred(streams_of[3], (TOKENS, HW), 1.0, 6.0, ((0, 4), (1, 8)))
    log_decay = draw_log_decay(jax.random.fold_in(streams_of[17], 71), 0)
    residual = centred(streams_of[5], (TOKENS, D), 1.0, 6.0, ((0, 32),))
    head_gain = jnp.clip(1.0 + 0.18 * jax.random.normal(streams_of[6], (HW,), jnp.float32), 0.1, 1.9)
    out_weight = centred(streams_of[7], (HW, D), HW ** -0.5, 0.1875, ((1, 8),))
    norm_gain = jnp.clip(1.0 + 0.18 * jax.random.normal(streams_of[8], (D,), jnp.float32), 0.1, 1.9)
    expert_ids_keys = jax.random.split(jax.random.fold_in(streams_of[9], 1), TOKENS // TOK_DEV)
    expert_ids_turns = jax.random.permutation(jax.random.fold_in(streams_of[9], 3), TOKENS // TOK_DEV)
    expert_ids = jax.vmap(lambda own, number: deal_out(jax.random.fold_in(streams_of[9], 2), own, number, TOK_DEV, SPECIALISTS, TOPK, CAP, 2))(expert_ids_keys, expert_ids_turns).reshape((TOKENS, TOPK))
    route_weights = jnp.clip(jnp.exp(math.log(1.0) - 1.609438 * jax.random.uniform(streams_of[10], (TOKENS, TOPK), jnp.float32) ** block_levels(streams_of[10], (TOKENS, TOPK), ((0, 32),), -0.2, 0.2)), 0.2, 1.0)
    expert_gate = centred(streams_of[11], (D, SPECIALISTS * FF), D ** -0.5, 0.125, ((1, 32),))
    expert_up = centred(streams_of[12], (D, SPECIALISTS * FF), D ** -0.5, 0.125, ((1, 32),))
    expert_down = centred(streams_of[13], (D, SPECIALISTS * FF), FF ** -0.5, 0.1875, ((1, 32),))
    shared_gate = centred(streams_of[14], (D, SH), D ** -0.5, 0.125)
    shared_up = centred(streams_of[15], (D, SH), D ** -0.5, 0.125)
    shared_down = centred(streams_of[16], (D, SH), SH ** -0.5, 0.25)
    return dict(query_rows=query_rows, key_rows=key_rows, value_rows=value_rows, gate_rows=gate_rows, log_decay=log_decay, residual=residual, head_gain=head_gain, out_weight=out_weight, norm_gain=norm_gain, expert_ids=expert_ids, route_weights=route_weights, expert_gate=expert_gate, expert_up=expert_up, expert_down=expert_down, shared_gate=shared_gate, shared_up=shared_up, shared_down=shared_down)


eps = 1e-05

def retain(queries, key_heads, values, log_decay):
    rows, heads, width = queries.shape
    count = rows // SPAN
    scale = width ** (-0.5)
    query_blocks = queries.reshape(count, SPAN, heads, width)
    key_blocks = key_heads.reshape(count, SPAN, heads, width)
    value_blocks = values.reshape(count, SPAN, heads, width)
    decay_blocks = log_decay.reshape(heads, count, SPAN).transpose(1, 0, 2)
    offsets = jnp.arange(SPAN, dtype=jnp.int32)
    causal = offsets[:, None] >= offsets[None, :]

    def advance(carry, inputs):
        block_queries, block_keys, block_values, decay_block = inputs
        query_matrix_full = block_queries.astype(jnp.float32)
        key_matrix_full = block_keys.astype(jnp.float32)
        value_matrix_full = block_values.astype(jnp.float32)
        running = jnp.cumsum(decay_block, axis=1)
        spread = running[:, :, None] - running[:, None, :]
        damping = jnp.exp(jnp.where(causal[None], spread, -jnp.inf))
        attention_scores = jnp.einsum('xru,jru->rxj', query_matrix_full, key_matrix_full)
        decay_weighted = lax.optimization_barrier((attention_scores * scale * damping).astype(jnp.bfloat16)).astype(jnp.float32)
        inner_block_term = jnp.einsum('svc,csj->vsj', decay_weighted, value_matrix_full)
        carried = jnp.einsum('nhd,hde->nhe', query_matrix_full, carry, precision=lax.Precision.HIGHEST)
        carried = carried * jnp.exp(running).T[:, :, None]
        decay_to_block_end = jnp.exp(running[:, -1:] - running).T[:, :, None] * scale
        state_update = jnp.einsum('jok,jow->okw', key_matrix_full * decay_to_block_end, value_matrix_full, precision=lax.Precision.HIGHEST)
        carry = carry * jnp.exp(running[:, -1])[:, None, None] + state_update
        return (carry, inner_block_term + carried)
    start = jnp.zeros((heads, width, width), jnp.float32)
    _, outputs = lax.scan(advance, start, (query_blocks, key_blocks, value_blocks, decay_blocks))
    return outputs.reshape(rows, heads, width)

def reference(query_rows, key_rows, value_rows, gate_rows, log_decay, residual, head_gain, out_weight, norm_gain, expert_ids, route_weights, expert_gate, expert_up, expert_down, shared_gate, shared_up, shared_down):
    retained = retain(query_rows.reshape(TOKENS, HEADS, HEAD), key_rows.reshape(TOKENS, HEADS, HEAD), value_rows.reshape(TOKENS, HEADS, HEAD), log_decay)
    centered = retained - lax.optimization_barrier(jnp.mean(retained, axis=2, keepdims=True))
    normed = centered * lax.rsqrt(lax.optimization_barrier(jnp.mean(centered * centered, axis=2, keepdims=True)) + eps)
    ret_rows = (normed.reshape(TOKENS, HW) * head_gain * jax.nn.silu(gate_rows.astype(jnp.float32))).astype(jnp.bfloat16)
    mixer = jnp.dot(ret_rows, out_weight, preferred_element_type=jnp.float32)
    hidden = (residual.astype(jnp.float32) + mixer).astype(jnp.bfloat16)
    hidden_wide = hidden.astype(jnp.float32)
    normed_rows = (hidden_wide * lax.rsqrt(lax.optimization_barrier(jnp.mean(hidden_wide * hidden_wide, axis=1, keepdims=True)) + eps) * norm_gain).astype(jnp.bfloat16)
    shared_mid = (jax.nn.silu(jnp.dot(normed_rows, shared_gate, preferred_element_type=jnp.float32)) * jnp.dot(normed_rows, shared_up, preferred_element_type=jnp.float32)).astype(jnp.bfloat16)
    shared_out = lax.dot_general(shared_mid, shared_down, (((1,), (1,)), ((), ())), preferred_element_type=jnp.float32)
    block_count = TOKENS // TOK_DEV
    slots = block_count * CAP
    block_index = jnp.arange(block_count, dtype=jnp.int32)[:, None]
    token_index = jnp.arange(TOKENS, dtype=jnp.int32)

    def expert_step(total, index):
        chosen = expert_ids == index
        picked = jnp.any(chosen, axis=1)
        weight = lax.optimization_barrier(jnp.sum(jnp.where(chosen, route_weights, 0.0), axis=1))
        blocked = picked.reshape(block_count, TOK_DEV).astype(jnp.int32)
        position = jnp.cumsum(blocked, axis=1) - 1
        target = jnp.where(blocked > 0, block_index * CAP + position, slots).reshape(-1).astype(jnp.int32)
        table = jnp.zeros((slots + 1,), jnp.int32).at[target].set(token_index)[:slots]
        live = jnp.zeros((slots + 1,), jnp.float32).at[target].set(1.0)[:slots]
        rows = normed_rows[table]
        gate_cols = lax.dynamic_slice_in_dim(expert_gate, index * FF, FF, 1)
        up_cols = lax.dynamic_slice_in_dim(expert_up, index * FF, FF, 1)
        down_cols = lax.dynamic_slice_in_dim(expert_down, index * FF, FF, 1)
        middle = (jax.nn.silu(jnp.dot(rows, gate_cols, preferred_element_type=jnp.float32)) * jnp.dot(rows, up_cols, preferred_element_type=jnp.float32)).astype(jnp.bfloat16)
        outcome = lax.dot_general(middle, down_cols, (((1,), (1,)), ((), ())), preferred_element_type=jnp.float32).astype(jnp.bfloat16)
        contrib = outcome.astype(jnp.float32) * (weight[table] * live)[:, None]
        return (total.at[table].add(contrib), None)
    routed, _ = lax.scan(expert_step, jnp.zeros((TOKENS, D), jnp.float32), jnp.arange(SPECIALISTS, dtype=jnp.int32))
    return (hidden_wide + routed + shared_out).astype(jnp.bfloat16)
```

```python
import functools

import jax
import jax.numpy as jnp
from jax import lax
from jax.experimental import pallas as pl
from jax.experimental.pallas import tpu as pltpu
from jax.sharding import PartitionSpec as P

HEAD = 64
BLOCK = 256
EXTRA = 8


eps = 1e-05
F32 = jnp.float32
BF16 = jnp.bfloat16


def split(value):
    high = value.astype(BF16)
    return high, (value - high.astype(F32)).astype(BF16)


def per_head(columns, lanes):
    heads = columns.shape[1]
    out = jnp.broadcast_to(columns[:, 0:1], lanes.shape)
    for head in range(1, heads):
        out = jnp.where(lanes // HEAD == head, columns[:, head : head + 1], out)
    return out


def gathered_update(keys, values, column, lanes, end):
    scale = HEAD ** (-0.5)
    weighted = keys.astype(F32) * (jnp.exp(per_head(end - column, lanes)) * scale)
    high, low = split(weighted)
    dims = (((0,), (0,)), ((), ()))
    return lax.dot_general(high, values, dims, preferred_element_type=F32) + lax.dot_general(
        low, values, dims, preferred_element_type=F32
    )


def state_kernel(key_ref, value_ref, column_ref, out_ref):
    width = key_ref.shape[1]
    step = pl.program_id(0)

    @pl.when(step == 0)
    def _():
        out_ref[0:width, :] = jnp.zeros((width, width), F32)
        out_ref[width:, :] = jnp.zeros((EXTRA, width), F32)

    lanes = lax.broadcasted_iota(jnp.int32, key_ref.shape, 1)
    column = column_ref[...]
    end = column[BLOCK - 1 : BLOCK, :]
    end_lanes = per_head(end, lanes[0:1, :])
    fresh = gathered_update(key_ref[...], value_ref[...], column, lanes, end)
    out_ref[0:width, :] = out_ref[0:width, :] * jnp.exp(end_lanes) + fresh
    out_ref[width:, :] = out_ref[width:, :] + end_lanes


def retention_kernel(
    mine_ref, query_ref, key_ref, value_ref, gate_ref, column_ref, row_ref, gain_ref, states_ref,
    out_ref, state
):
    rows, width = query_ref.shape
    heads = width // HEAD
    step = pl.program_id(0)
    count = states_ref.shape[0]
    row_ids = lax.broadcasted_iota(jnp.int32, (width, width), 0) // HEAD
    column_ids = lax.broadcasted_iota(jnp.int32, (width, width), 1) // HEAD

    @pl.when(step == 0)
    def _():
        total = jnp.zeros((width, width), F32)
        for position in range(count - 1):
            decay = jnp.exp(states_ref[position, width : width + 1, :])
            longer = total * decay + states_ref[position, 0:width, :]
            total = jnp.where(position < mine_ref[0], longer, total)
        state[...] = jnp.where(row_ids == column_ids, total, 0.0)

    lanes = lax.broadcasted_iota(jnp.int32, (rows, width), 1)
    queries, keys, values = query_ref[...], key_ref[...], value_ref[...]
    column = column_ref[...]
    end = column[rows - 1 : rows, :]
    causal = lax.broadcasted_iota(jnp.int32, (rows, rows), 0) >= lax.broadcasted_iota(
        jnp.int32, (rows, rows), 1
    )
    scale = HEAD ** (-0.5)
    high, low = split(state[...])
    carried = jnp.dot(queries, high, preferred_element_type=F32) + jnp.dot(
        queries, low, preferred_element_type=F32
    )
    retained = carried * jnp.exp(per_head(column, lanes))
    inner = None
    for head in range(heads):
        own = jnp.where(lanes // HEAD == head, queries.astype(F32), 0.0).astype(BF16)
        scores = lax.dot_general(
            own, keys, (((1,), (1,)), ((), ())), preferred_element_type=F32
        )
        spread = column[:, head : head + 1] - row_ref[0, head : head + 1, :]
        damping = jnp.exp(jnp.where(causal, spread, -jnp.inf))
        factor = (scores * scale * damping).astype(BF16)
        term = jnp.dot(factor, values, preferred_element_type=F32)
        inner = term if inner is None else jnp.where(lanes // HEAD == head, term, inner)
    retained = retained + inner
    fresh = gathered_update(keys, values, column, lanes, end)
    end_lanes = per_head(end, lanes[0:1, :])
    state[...] = state[...] * jnp.exp(end_lanes) + jnp.where(row_ids == column_ids, fresh, 0.0)

    def head_mean(array):
        out = None
        for head in range(heads):
            inside = lanes // HEAD == head
            mean = jnp.sum(jnp.where(inside, array, 0.0), axis=1, keepdims=True) * (1.0 / HEAD)
            out = jnp.broadcast_to(mean, array.shape) if out is None else jnp.where(inside, mean, out)
        return out

    centered = retained - head_mean(retained)
    normed = centered * lax.rsqrt(head_mean(centered * centered) + eps)
    gates = gate_ref[...].astype(F32)
    out_ref[...] = (normed * gain_ref[...] * (gates * jax.nn.sigmoid(gates))).astype(BF16)


def retention(query_rows, key_rows, value_rows, gate_rows, log_decay, head_gain):
    rows, width = query_rows.shape
    heads = width // HEAD
    count = rows // BLOCK
    running = jnp.cumsum(log_decay.reshape(heads, count, BLOCK), axis=2)
    row = running.transpose(1, 0, 2)
    column = running.reshape(heads, rows).T
    block = pl.BlockSpec((BLOCK, width), lambda i: (i, 0))
    column_block = pl.BlockSpec((BLOCK, heads), lambda i: (i, 0))
    own = pl.pallas_call(
        state_kernel,
        grid=(count,),
        in_specs=[block, block, column_block],
        out_specs=pl.BlockSpec((width + EXTRA, width), lambda i: (0, 0)),
        out_shape=jax.ShapeDtypeStruct((width + EXTRA, width), F32),
        compiler_params=pltpu.CompilerParams(dimension_semantics=("arbitrary",)),
        cost_estimate=pl.CostEstimate(
            flops=4 * rows * width * width, bytes_accessed=4 * rows * width, transcendentals=rows * width
        ),
    )(key_rows, value_rows, column)
    states = lax.all_gather(own, "sp")
    mine = lax.axis_index("sp").astype(jnp.int32).reshape(1)
    return pl.pallas_call(
        retention_kernel,
        grid=(count,),
        in_specs=[
            pl.BlockSpec(memory_space=pltpu.SMEM),
            block,
            block,
            block,
            block,
            column_block,
            pl.BlockSpec((1, heads, BLOCK), lambda i: (i, 0, 0)),
            pl.BlockSpec((1, width), lambda i: (0, 0)),
            pl.BlockSpec(states.shape, lambda i: (0, 0, 0)),
        ],
        out_specs=block,
        out_shape=jax.ShapeDtypeStruct((rows, width), BF16),
        scratch_shapes=[pltpu.VMEM((width, width), F32)],
        compiler_params=pltpu.CompilerParams(dimension_semantics=("arbitrary",)),
        cost_estimate=pl.CostEstimate(
            flops=8 * rows * width * BLOCK,
            bytes_accessed=10 * rows * width,
            transcendentals=rows * BLOCK * heads,
        ),
    )(mine, query_rows, key_rows, value_rows, gate_rows, column, row, head_gain[None, :], states)


def both_halves(weight):
    size = lax.axis_size("tp")
    groups = [list(range(core, size, 2)) for core in range(2)]
    half = lax.all_gather(weight, "tp", axis=1, tiled=True, axis_index_groups=groups)
    other = lax.ppermute(half, "tp", [(i, i ^ 1) for i in range(size)])
    return half, other


def on_device(
    query_rows,
    key_rows,
    value_rows,
    gate_rows,
    log_decay,
    residual,
    head_gain,
    out_weight,
    norm_gain,
    expert_ids,
    route_weights,
    expert_gate,
    expert_up,
    expert_down,
    shared_gate,
    shared_up,
    shared_down,
):
    out_half, out_other = both_halves(out_weight)
    gates, ups, downs = both_halves(expert_gate), both_halves(expert_up), both_halves(expert_down)

    specialists = lax.axis_size("sp")
    tokens, chosen = expert_ids.shape
    width = residual.shape[1]
    capacity = 3 * tokens * chosen // (2 * specialists)
    names = jnp.arange(specialists, dtype=jnp.int32)[:, None]
    named = [expert_ids[:, j][None, :] == names for j in range(chosen)]
    match = functools.reduce(jnp.logical_or, named)
    weight = sum(jnp.where(named[j], route_weights[:, j][None, :], 0.0) for j in range(chosen))
    earlier = jnp.arange(tokens)[:, None] < jnp.arange(tokens)[None, :]
    position = jnp.dot(match.astype(BF16), earlier.astype(BF16), preferred_element_type=F32)
    place = jnp.where(match, position.astype(jnp.int32), -1)
    sits = place[:, None, :] == jnp.arange(capacity, dtype=jnp.int32)[None, :, None]
    pick = sits.astype(BF16).reshape(specialists * capacity, tokens)
    weight_high = lax.reduce_precision(weight, 8, 7)
    weight_low = weight - weight_high
    back_high = jnp.where(sits, weight_high[:, None, :], 0.0).astype(BF16)
    back_low = jnp.where(sits, weight_low[:, None, :], 0.0).astype(BF16)

    ret_rows = retention(query_rows, key_rows, value_rows, gate_rows, log_decay, head_gain)
    token_rows = lax.all_to_all(ret_rows, "tp", split_axis=0, concat_axis=1, tiled=True)
    mine = jnp.dot(token_rows, out_half, preferred_element_type=F32)
    others = jnp.dot(token_rows, out_other, preferred_element_type=F32)
    core = lax.axis_index("tp") % 2
    piece = out_weight.shape[1]
    mine, others = mine.reshape(tokens, -1, piece), others.reshape(tokens, -1, piece)
    mixer = jnp.stack(
        [jnp.where(core == 0, mine, others), jnp.where(core == 0, others, mine)], axis=2
    ).reshape(tokens, width)
    hidden = (residual.astype(F32) + mixer).astype(BF16)
    hidden_wide = hidden.astype(F32)
    normed_rows = (
        hidden_wide
        * lax.rsqrt(jnp.mean(hidden_wide * hidden_wide, axis=1, keepdims=True) + eps)
        * norm_gain
    ).astype(BF16)
    outgoing = jnp.dot(pick, normed_rows, preferred_element_type=F32).astype(BF16)
    outgoing = outgoing.reshape(specialists, capacity, width)
    arrived = lax.all_to_all(outgoing, "sp", split_axis=0, concat_axis=0, tiled=True)
    shared_mid = (
        jax.nn.silu(jnp.dot(normed_rows, shared_gate, preferred_element_type=F32))
        * jnp.dot(normed_rows, shared_up, preferred_element_type=F32)
    ).astype(BF16)
    shared_out = lax.dot_general(
        shared_mid, shared_down, (((1,), (1,)), ((), ())), preferred_element_type=F32
    )
    flat_rows = arrived.reshape(-1, width)
    outcome = 0.0
    for gate, up, down in zip(gates, ups, downs):
        middle = (
            jax.nn.silu(jnp.dot(flat_rows, gate, preferred_element_type=F32))
            * jnp.dot(flat_rows, up, preferred_element_type=F32)
        ).astype(BF16)
        outcome += lax.dot_general(
            middle, down, (((1,), (1,)), ((), ())), preferred_element_type=F32
        )
    processed = outcome.astype(BF16).reshape(arrived.shape)
    returned = lax.all_to_all(processed, "sp", split_axis=0, concat_axis=0, tiled=True)
    dims = (((0, 1), (0, 1)), ((), ()))
    routed = lax.dot_general(back_high, returned, dims, preferred_element_type=F32)
    routed += lax.dot_general(back_low, returned, dims, preferred_element_type=F32)
    return (hidden_wide + routed + shared_out).astype(BF16)


def solution(mesh):
    placed = (
        P("sp", "tp"),
        P("sp", "tp"),
        P("sp", "tp"),
        P("sp", "tp"),
        P("tp", "sp"),
        P(("sp", "tp"), None),
        P("tp"),
        P(None, "tp"),
        P(),
        P(("sp", "tp"), None),
        P(("sp", "tp"), None),
        P(None, ("sp", "tp")),
        P(None, ("sp", "tp")),
        P(None, ("sp", "tp")),
        P(),
        P(),
        P(),
    )
    return jax.shard_map(
        on_device, mesh=mesh, in_specs=placed, out_specs=P(("sp", "tp"), None), check_vma=False
    )
```

```python
import functools

import jax
import jax.numpy as jnp
from jax import lax
from jax.experimental import pallas as pl
from jax.experimental.pallas import tpu as pltpu
from jax.sharding import PartitionSpec as P


HEAD = 64
BLOCK = 256
EXTRA = 8


eps = 1e-05
F32 = jnp.float32
BF16 = jnp.bfloat16


def split(value):
    high = value.astype(BF16)
    return high, (value - high.astype(F32)).astype(BF16)


def per_head(columns, lanes):
    heads = columns.shape[1]
    out = jnp.broadcast_to(columns[:, 0:1], lanes.shape)
    for head in range(1, heads):
        out = jnp.where(lanes // HEAD == head, columns[:, head : head + 1], out)
    return out


def gathered_update(keys, values, column, lanes, end):
    scale = HEAD ** (-0.5)
    weighted = keys.astype(F32) * (jnp.exp(per_head(end - column, lanes)) * scale)
    high, low = split(weighted)
    dims = (((0,), (0,)), ((), ()))
    return lax.dot_general(high, values, dims, preferred_element_type=F32) + lax.dot_general(
        low, values, dims, preferred_element_type=F32
    )


def state_kernel(key_ref, value_ref, column_ref, out_ref):
    width = key_ref.shape[1]
    step = pl.program_id(0)

    @pl.when(step == 0)
    def _():
        out_ref[0:width, :] = jnp.zeros((width, width), F32)
        out_ref[width:, :] = jnp.zeros((EXTRA, width), F32)

    lanes = lax.broadcasted_iota(jnp.int32, key_ref.shape, 1)
    column = column_ref[...]
    end = column[BLOCK - 1 : BLOCK, :]
    end_lanes = per_head(end, lanes[0:1, :])
    fresh = gathered_update(key_ref[...], value_ref[...], column, lanes, end)
    out_ref[0:width, :] = out_ref[0:width, :] * jnp.exp(end_lanes) + fresh
    out_ref[width:, :] = out_ref[width:, :] + end_lanes


def retention_kernel(
    mine_ref, query_ref, key_ref, value_ref, gate_ref, column_ref, row_ref, gain_ref, states_ref,
    out_ref, state
):
    rows, width = query_ref.shape
    heads = width // HEAD
    step = pl.program_id(0)
    count = states_ref.shape[0]
    row_ids = lax.broadcasted_iota(jnp.int32, (width, width), 0) // HEAD
    column_ids = lax.broadcasted_iota(jnp.int32, (width, width), 1) // HEAD

    @pl.when(step == 0)
    def _():
        total = jnp.zeros((width, width), F32)
        for position in range(count - 1):
            decay = jnp.exp(states_ref[position, width : width + 1, :])
            longer = total * decay + states_ref[position, 0:width, :]
            total = jnp.where(position < mine_ref[0], longer, total)
        state[...] = jnp.where(row_ids == column_ids, total, 0.0)

    lanes = lax.broadcasted_iota(jnp.int32, (rows, width), 1)
    queries, keys, values = query_ref[...], key_ref[...], value_ref[...]
    column = column_ref[...]
    end = column[rows - 1 : rows, :]
    causal = lax.broadcasted_iota(jnp.int32, (rows, rows), 0) >= lax.broadcasted_iota(
        jnp.int32, (rows, rows), 1
    )
    scale = HEAD ** (-0.5)
    high, low = split(state[...])
    carried = jnp.dot(queries, high, preferred_element_type=F32) + jnp.dot(
        queries, low, preferred_element_type=F32
    )
    retained = carried * jnp.exp(per_head(column, lanes))
    inner = None
    for head in range(heads):
        own = jnp.where(lanes // HEAD == head, queries.astype(F32), 0.0).astype(BF16)
        scores = lax.dot_general(
            own, keys, (((1,), (1,)), ((), ())), preferred_element_type=F32
        )
        spread = column[:, head : head + 1] - row_ref[0, head : head + 1, :]
        damping = jnp.exp(jnp.where(causal, spread, -jnp.inf))
        factor = (scores * scale * damping).astype(BF16)
        term = jnp.dot(factor, values, preferred_element_type=F32)
        inner = term if inner is None else jnp.where(lanes // HEAD == head, term, inner)
    retained = retained + inner
    fresh = gathered_update(keys, values, column, lanes, end)
    end_lanes = per_head(end, lanes[0:1, :])
    state[...] = state[...] * jnp.exp(end_lanes) + jnp.where(row_ids == column_ids, fresh, 0.0)

    def head_mean(array):
        out = None
        for head in range(heads):
            inside = lanes // HEAD == head
            mean = jnp.sum(jnp.where(inside, array, 0.0), axis=1, keepdims=True) * (1.0 / HEAD)
            out = jnp.broadcast_to(mean, array.shape) if out is None else jnp.where(inside, mean, out)
        return out

    centered = retained - head_mean(retained)
    normed = centered * lax.rsqrt(head_mean(centered * centered) + eps)
    gates = gate_ref[...].astype(F32)
    out_ref[...] = (normed * gain_ref[...] * (gates * jax.nn.sigmoid(gates))).astype(BF16)


def retention(query_rows, key_rows, value_rows, gate_rows, log_decay, head_gain):
    rows, width = query_rows.shape
    heads = width // HEAD
    count = rows // BLOCK
    running = jnp.cumsum(log_decay.reshape(heads, count, BLOCK), axis=2)
    row = running.transpose(1, 0, 2)
    column = running.reshape(heads, rows).T
    block = pl.BlockSpec((BLOCK, width), lambda i: (i, 0))
    column_block = pl.BlockSpec((BLOCK, heads), lambda i: (i, 0))
    state_call = pl.pallas_call(
        state_kernel,
        grid=(count,),
        in_specs=[block, block, column_block],
        out_specs=pl.BlockSpec((width + EXTRA, width), lambda i: (0, 0)),
        out_shape=jax.ShapeDtypeStruct((width + EXTRA, width), F32),
        compiler_params=pltpu.CompilerParams(dimension_semantics=("arbitrary",)),
        cost_estimate=pl.CostEstimate(
            flops=4 * rows * width * width, bytes_accessed=4 * rows * width, transcendentals=rows * width
        ),
    )
    own = state_call(key_rows, value_rows, column)
    states = lax.all_gather(own, "sp")
    mine = lax.axis_index("sp").astype(jnp.int32).reshape(1)
    return pl.pallas_call(
        retention_kernel,
        grid=(count,),
        in_specs=[
            pl.BlockSpec(memory_space=pltpu.SMEM),
            block,
            block,
            block,
            block,
            column_block,
            pl.BlockSpec((1, heads, BLOCK), lambda i: (i, 0, 0)),
            pl.BlockSpec((1, width), lambda i: (0, 0)),
            pl.BlockSpec(states.shape, lambda i: (0, 0, 0)),
        ],
        out_specs=block,
        out_shape=jax.ShapeDtypeStruct((rows, width), BF16),
        scratch_shapes=[pltpu.VMEM((width, width), F32)],
        compiler_params=pltpu.CompilerParams(dimension_semantics=("arbitrary",)),
        cost_estimate=pl.CostEstimate(
            flops=8 * rows * width * BLOCK,
            bytes_accessed=10 * rows * width,
            transcendentals=rows * BLOCK * heads,
        ),
    )(mine, query_rows, key_rows, value_rows, gate_rows, column, row, head_gain[None, :], states)


def send(piece, pairs):
    return lax.ppermute(piece, "tp", pairs)


def ring_start(own):
    size = lax.axis_size("tp")
    right = [(i, (i + 2) % size) for i in range(size)]
    left = [(i, (i - 2) % size) for i in range(size)]
    swap = [(i, i ^ 1) for i in range(size)]
    return send(own, right), send(own, left), send(own, swap)


def ring_finish(own, from_left, from_right, other):
    size = lax.axis_size("tp")
    chips = size // 2
    right = [(i, (i + 2) % size) for i in range(size)]
    left = [(i, (i - 2) % size) for i in range(size)]
    swap = [(i, i ^ 1) for i in range(size)]
    half = own.shape[1] // 2
    last = chips // 2
    pieces = [[own], [other]]
    for hop in range(1, (chips - 1) // 2 + 1):
        if hop > 1:
            from_left = send(from_left, right)
            from_right = send(from_right, left)
        for piece in (from_left, from_right):
            pieces += [[piece], [send(piece, swap)]]
    if chips % 2 == 0 and last > 1:
        first = send(from_left[:, :half], right)
        second = send(from_right[:, half:], left)
        pieces += [[first, second], [send(first, swap), send(second, swap)]]
    elif chips == 2:
        pieces += [[from_left], [send(from_left, swap)]]
    return pieces


def expert_kernel(layout, row_ref, *refs):
    count = len(layout)
    piece_refs, out_ref = refs[:count], refs[count]
    weights, middle, sems = refs[count + 1 :]
    slots, _, width, ff = weights.shape
    rows = row_ref.shape[0]
    copies = []
    for index, (slot, start, length) in enumerate(layout):
        copy = pltpu.make_async_copy(
            piece_refs[index], weights.at[slot, :, pl.ds(start, length), :], sems.at[index]
        )
        copy.start()
        copies.append(copy)
    tile = rows // 2
    for pair in range(slots // 2):
        for index, (slot, _, _) in enumerate(layout):
            if slot // 2 == pair:
                copies[index].wait()

        @pl.loop(0, 2)
        def _(step):
            span = pl.ds(pl.multiple_of(step * tile, tile), tile)
            block = row_ref[span, :]
            gate = jnp.concatenate([weights[2 * pair, 0], weights[2 * pair + 1, 0]], axis=1)
            up = jnp.concatenate([weights[2 * pair, 1], weights[2 * pair + 1, 1]], axis=1)
            gated = jnp.dot(block, gate, preferred_element_type=F32)
            raised = jnp.dot(block, up, preferred_element_type=F32)
            value = gated * jax.nn.sigmoid(gated) * raised
            middle[span, 2 * pair * ff : 2 * (pair + 1) * ff] = value.astype(BF16)

    part = 512

    @pl.loop(0, width // part)
    def _(step):
        span = pl.ds(pl.multiple_of(step * part, part), part)
        down = jnp.concatenate([weights[slot, 2, span, :] for slot in range(slots)], axis=1)
        out_ref[:, span] = lax.dot_general(
            middle[...], down, (((1,), (1,)), ((), ())), preferred_element_type=F32
        ).astype(BF16)


def experts(rows, shards):
    _, width, ff = shards[0][0].shape
    count = len(shards)
    if ff % 128 or count % 2:
        whole = jnp.concatenate([jnp.concatenate(shard, axis=1) for shard in shards], axis=2)
        middle = (
            jax.nn.silu(jnp.dot(rows, whole[0], preferred_element_type=F32))
            * jnp.dot(rows, whole[1], preferred_element_type=F32)
        ).astype(BF16)
        return lax.dot_general(
            middle, whole[2], (((1,), (1,)), ((), ())), preferred_element_type=F32
        ).astype(BF16)
    layout, pieces = [], []
    for slot, shard in enumerate(shards):
        start = 0
        for piece in shard:
            layout.append((slot, start, piece.shape[1]))
            pieces.append(piece)
            start += piece.shape[1]
    return pl.pallas_call(
        functools.partial(expert_kernel, layout),
        in_specs=[pl.BlockSpec(memory_space=pltpu.VMEM)]
        + [pl.BlockSpec(memory_space=pl.ANY)] * len(pieces),
        out_specs=pl.BlockSpec(memory_space=pltpu.VMEM),
        out_shape=jax.ShapeDtypeStruct(rows.shape, BF16),
        scratch_shapes=[
            pltpu.VMEM((count, 3, width, ff), BF16),
            pltpu.VMEM((rows.shape[0], count * ff), BF16),
            pltpu.SemaphoreType.DMA((len(pieces),)),
        ],
        compiler_params=pltpu.CompilerParams(vmem_limit_bytes=60 * 1024 * 1024),
        cost_estimate=pl.CostEstimate(
            flops=6 * rows.shape[0] * width * count * ff,
            bytes_accessed=6 * width * count * ff + 4 * rows.size,
            transcendentals=rows.shape[0] * count * ff,
        ),
    )(rows, *pieces)


def on_device(
    query_rows,
    key_rows,
    value_rows,
    gate_rows,
    log_decay,
    residual,
    head_gain,
    out_weight,
    norm_gain,
    expert_ids,
    route_weights,
    expert_gate,
    expert_up,
    expert_down,
    shared_gate,
    shared_up,
    shared_down,
):
    out_full = lax.all_gather(out_weight, "tp", axis=1, tiled=True)
    shard = jnp.stack([expert_gate, expert_up, expert_down])
    shard, log_decay = lax.optimization_barrier((shard, log_decay))
    from_left, from_right, other = ring_start(shard)

    specialists = lax.axis_size("sp")
    tokens, chosen = expert_ids.shape
    width = residual.shape[1]
    capacity = 3 * tokens * chosen // (2 * specialists)
    names = jnp.arange(specialists, dtype=jnp.int32)[:, None]
    named = [expert_ids[:, j][None, :] == names for j in range(chosen)]
    match = functools.reduce(jnp.logical_or, named)
    weight = sum(jnp.where(named[j], route_weights[:, j][None, :], 0.0) for j in range(chosen))
    earlier = jnp.arange(tokens)[:, None] < jnp.arange(tokens)[None, :]
    position = jnp.dot(match.astype(BF16), earlier.astype(BF16), preferred_element_type=F32)
    place = jnp.where(match, position.astype(jnp.int32), -1)
    sits = place[:, None, :] == jnp.arange(capacity, dtype=jnp.int32)[None, :, None]
    pick = sits.astype(BF16).reshape(specialists * capacity, tokens)
    weight_high = lax.reduce_precision(weight, 8, 7)
    weight_low = weight - weight_high
    back_high = jnp.where(sits, weight_high[:, None, :], 0.0).astype(BF16)
    back_low = jnp.where(sits, weight_low[:, None, :], 0.0).astype(BF16)

    ret_rows = retention(query_rows, key_rows, value_rows, gate_rows, log_decay, head_gain)
    token_rows = lax.all_to_all(ret_rows, "tp", split_axis=0, concat_axis=1, tiled=True)
    token_rows, from_left, from_right = lax.optimization_barrier((token_rows, from_left, from_right))
    shards = ring_finish(shard, from_left, from_right, other)
    mixer = jnp.dot(token_rows, out_full, preferred_element_type=F32)
    hidden = (residual.astype(F32) + mixer).astype(BF16)
    hidden_wide = hidden.astype(F32)
    normed_rows = (
        hidden_wide
        * lax.rsqrt(jnp.mean(hidden_wide * hidden_wide, axis=1, keepdims=True) + eps)
        * norm_gain
    ).astype(BF16)
    outgoing = jnp.dot(pick, normed_rows, preferred_element_type=F32).astype(BF16)
    outgoing = outgoing.reshape(specialists, capacity, width)
    arrived = lax.all_to_all(outgoing, "sp", split_axis=0, concat_axis=0, tiled=True)
    shared_mid = (
        jax.nn.silu(jnp.dot(normed_rows, shared_gate, preferred_element_type=F32))
        * jnp.dot(normed_rows, shared_up, preferred_element_type=F32)
    ).astype(BF16)
    shared_out = lax.dot_general(
        shared_mid, shared_down, (((1,), (1,)), ((), ())), preferred_element_type=F32
    )
    flat_rows = arrived.reshape(-1, width)
    processed = experts(flat_rows, shards).reshape(arrived.shape)
    returned = lax.all_to_all(processed, "sp", split_axis=0, concat_axis=0, tiled=True)
    dims = (((0, 1), (0, 1)), ((), ()))
    routed = lax.dot_general(back_high, returned, dims, preferred_element_type=F32)
    routed += lax.dot_general(back_low, returned, dims, preferred_element_type=F32)
    return (hidden_wide + routed + shared_out).astype(BF16)


def solution(mesh):
    placed = (
        P("sp", "tp"),
        P("sp", "tp"),
        P("sp", "tp"),
        P("sp", "tp"),
        P("tp", "sp"),
        P(("sp", "tp"), None),
        P("tp"),
        P(None, "tp"),
        P(),
        P(("sp", "tp"), None),
        P(("sp", "tp"), None),
        P(None, ("sp", "tp")),
        P(None, ("sp", "tp")),
        P(None, ("sp", "tp")),
        P(),
        P(),
        P(),
    )

    return jax.shard_map(
        on_device, mesh=mesh, in_specs=placed, out_specs=P(("sp", "tp"), None), check_vma=False
    )
```
